32 devices in a mesh: sp: 4 (over y, x), tp: 8 (over z, core).
Axes of the slice: x: 2, y: 2, z: 4, core: 2. Of those that a mesh axis runs over, the one named last changes fastest.
Arguments:
- queries: bfloat16 [4096, 2048], P('sp', 'tp'), may hold values from -8 to 8
- keys: bfloat16 [4096, 512], P('sp'), may hold values from -6 to 6
- values: bfloat16 [4096, 512], P('sp'), may hold values from -6 to 6
- query_gain: float32 [2048], P('tp'), may hold values from 0.2 to 40
- key_gain: float32 [128], replicated, may hold values from 0.1 to 1.9
- out_weight: bfloat16 [2048, 2048], replicated, may hold values from -0.125 to 0.125
- residual: bfloat16 [4096, 2048], P(('sp', 'tp')), may hold values from -2 to 2
- norm_gain: float32 [2048], replicated, may hold values from 0.1 to 1.9
- route_experts: int32 [4096, 2], P(('sp', 'tp')), may hold values from 0 to 3, as said below
- expert_scores: float32 [4096, 2], P(('sp', 'tp')), may hold values from -9 to 9
- group_prob: float32 [4096], P(('sp', 'tp')), may hold values from 0.5 to 1
- w_gate: bfloat16 [4, 2048, 2048], P('sp', None, 'tp'), may hold values from -0.125 to 0.125
- w_up: bfloat16 [4, 2048, 2048], P('sp', None, 'tp'), may hold values from -0.125 to 0.125
- w_down: bfloat16 [4, 2048, 2048], P('sp', 'tp'), may hold values from -0.125 to 0.125
Outputs:
- mixed: bfloat16 [4096, 2048], P(('sp', 'tp'))
The draws below stay inside these ranges and needn't reach their ends.
Inputs may be any that keep to these rules, and one draw needn't show every extreme that they name: `route_experts`: each row names 2 different experts of one group, expert e lying in group e // 2. In the rows of one device (aligned blocks of 128 rows) 5 * 16 rows choose one group and the others another; inside a group those rows are spread over its experts as evenly as whole numbers allow, so no expert is named by more than 80 rows of one device and some expert by exactly 80.
All inputs are finite; a program needn't handle non-finite values.
Results may differ from the reference program's by a relative error of at most 0.025.
Values may be sent and summed in bfloat16 or wider, within the bound.
A program may use at most 128 MiB of HBM per device.

```python
import math
import jax
import jax.numpy as jnp
from jax import lax

D = 2048
HEADS = 16
KV_HEADS = 4
HEAD = 128
EXPERT_HIDDEN = 2048
GROUPS = 2
TOP = 2
GRID_W = 64
TOKENS = 4096
ROWS = 128
EXPERTS = 4
GROUP_EXPERTS = 2
UNIT_BLOCK = 256
CAP = 80
N_SP = 4
N_TP = 8


def key_field(key):
    drawn = jax.random.normal(jax.random.fold_in(key, 101), (TOKENS, KV_HEADS * HEAD), jnp.float32)
    return jnp.clip(drawn, -6.0, 6.0)


def draw_keys(key, part):
    return key_field(key).astype(jnp.bfloat16)


def draw_queries(key, part):
    anchor = jax.random.fold_in(key, 202)
    drawn = jax.random.normal(anchor, (TOKENS, HEADS * HEAD), jnp.float32)
    return jnp.clip(drawn, -6.0, 6.0).astype(jnp.bfloat16)


def draw_query_gain(key, part):
    level = jax.random.uniform(jax.random.fold_in(key, 301), (HEADS, 1), jnp.float32, math.log(1.2), math.log(3.0))
    jitter = 1.0 + 0.18 * jnp.clip(jax.random.normal(jax.random.fold_in(key, 302), (HEADS, HEAD), jnp.float32), -3.0, 3.0)
    return (jnp.exp(level) * jitter).reshape(HEADS * HEAD)


def draw_residual(key, part):
    columns = jnp.exp(jax.random.uniform(jax.random.fold_in(key, 401), (1, D), jnp.float32, math.log(0.3), math.log(3.0)))
    vectors = jnp.clip(jax.random.normal(jax.random.fold_in(key, 403), (TOKENS, D), jnp.float32), -6.0, 6.0)
    return (0.1 * vectors * columns).astype(jnp.bfloat16)


def route_block(block_key):
    order = jax.random.permutation(jax.random.fold_in(block_key, 1), ROWS)
    ranking = jnp.argsort(order).astype(jnp.int32)
    big_group = jax.random.randint(jax.random.fold_in(block_key, 2), (), 0, GROUPS)
    offset = jax.random.randint(jax.random.fold_in(block_key, 4), (), 0, GROUPS - 1)
    small_group = (big_group + 1 + offset) % GROUPS
    big_count = 5 * ROWS // 8
    in_big = ranking < big_count
    member = jnp.where(in_big, ranking, ranking - big_count)
    group_of = jnp.where(in_big, big_group, small_group)
    round_count = TOP * ROWS // GROUP_EXPERTS + 2
    round_keys = jax.random.split(jax.random.fold_in(block_key, 3), round_count)
    table = jax.vmap(lambda round_key: jax.random.permutation(round_key, GROUP_EXPERTS))(round_keys)
    first_place = TOP * member
    local = jnp.stack([table[(first_place + choice_rank) // GROUP_EXPERTS, (first_place + choice_rank) % GROUP_EXPERTS] for choice_rank in range(TOP)], axis=1)
    return group_of[:, None] * GROUP_EXPERTS + local


def draw_route_experts(key, part):
    block_total = TOKENS // ROWS
    block_keys = jax.random.split(jax.random.fold_in(key, 501), block_total)
    return jax.vmap(route_block)(block_keys).reshape(TOKENS, TOP).astype(jnp.int32)


def block_scale(own_key, dims, cuts, low, high):
    factor_of, own = 1.0, jax.random.fold_in(own_key, 6)
    for dim, parts in cuts:
        draws = jnp.exp(jax.random.uniform(jax.random.fold_in(own, dim), (parts,), jnp.float32, low / len(cuts), high / len(cuts)))
        factor_of = factor_of * jnp.repeat(draws, dims[dim] // parts).reshape([-1 if axis == dim else 1 for axis in range(len(dims))])
    return factor_of


def centred(own_key, dims, scale, bound, shards=(), kind=jnp.bfloat16):
    entries = jax.random.normal(own_key, dims, jnp.float32) * scale
    if len(shards) > 0:
        entries = block_scale(own_key, dims, shards, -0.22, 0.18) * entries
    return jnp.clip(entries, min=-bound, max=bound).astype(kind)


def setup_inputs(seed: int = 0) -> dict:
    seeds = jax.random.split(jax.random.key(seed), 15)
    queries = draw_queries(jax.random.fold_in(seeds[14], 71), 0)
    keys = draw_keys(jax.random.fold_in(seeds[14], 71), 0)
    values = centred(seeds[2], (TOKENS, KV_HEADS * HEAD), 1.0, 6.0, ((0, 4),))
    query_gain = draw_query_gain(jax.random.fold_in(seeds[14], 71), 0)
    key_gain = jnp.clip(1.0 + 0.18 * jax.random.normal(seeds[4], (HEAD,), jnp.float32), 0.1, 1.9)
    out_weight = centred(seeds[5], (HEADS * HEAD, D), (HEADS * HEAD) ** -0.5, 0.125)
    residual = draw_residual(jax.random.fold_in(seeds[14], 71), 0)
    norm_gain = jnp.clip(1.0 + 0.18 * jax.random.normal(seeds[7], (D,), jnp.float32), 0.1, 1.9)
    route_experts = draw_route_experts(jax.random.fold_in(seeds[14], 71), 0)
    expert_scores = centred(seeds[9], (TOKENS, TOP), 1.5, 9.0, ((0, 32),), jnp.float32)
    group_prob = jnp.clip(0.5 + 0.5 * jax.random.uniform(seeds[10], (TOKENS,), jnp.float32) ** block_scale(seeds[10], (TOKENS,), ((0, 32),), -0.2, 0.2), 0.5, 1.0)
    w_gate = centred(seeds[11], (EXPERTS, D, EXPERT_HIDDEN), D ** -0.5, 0.125, ((0, 4), (2, 8)))
    w_up = centred(seeds[12], (EXPERTS, D, EXPERT_HIDDEN), D ** -0.5, 0.125, ((0, 4), (2, 8)))
    w_down = centred(seeds[13], (EXPERTS, EXPERT_HIDDEN, D), EXPERT_HIDDEN ** -0.5, 0.125, ((0, 4), (1, 8)))
    return dict(queries=queries, keys=keys, values=values, query_gain=query_gain, key_gain=key_gain, out_weight=out_weight, residual=residual, norm_gain=norm_gain, route_experts=route_experts, expert_scores=expert_scores, group_prob=group_prob, w_gate=w_gate, w_up=w_up, w_down=w_down)


rope_base = 10000.0
norm_eps = 1e-06
query_block = 128

def rope_tables(positions, head_size):
    quarter = head_size // 4
    frequency = rope_base ** (-jnp.arange(quarter, dtype=jnp.float32) * 4.0 / head_size)
    grid_row = (positions // GRID_W).astype(jnp.float32)
    grid_column = (positions % GRID_W).astype(jnp.float32)
    angles = jnp.concatenate([grid_row[:, None] * frequency[None, :], grid_column[:, None] * frequency[None, :]], axis=1)
    return (jnp.cos(angles), jnp.sin(angles))

def rotate_pairs(vectors, cosine_table, sine_table):
    paired = vectors.reshape(vectors.shape[0], vectors.shape[1], vectors.shape[2] // 2, 2)
    leading = paired[..., 0]
    trailing = paired[..., 1]
    cosine_now = cosine_table[:, None, :]
    sine_now = sine_table[:, None, :]
    turned = jnp.stack([leading * cosine_now - trailing * sine_now, leading * sine_now + trailing * cosine_now], axis=-1)
    return turned.reshape(vectors.shape)

def head_norm(vectors, gain_row):
    factor = lax.rsqrt(lax.optimization_barrier(jnp.mean(vectors * vectors, axis=-1, keepdims=True)) + norm_eps)
    return vectors * factor * gain_row

def reference(queries, keys, values, query_gain, key_gain, out_weight, residual, norm_gain, route_experts, expert_scores, group_prob, w_gate, w_up, w_down):
    token_count = queries.shape[0]
    positions = jnp.arange(token_count, dtype=jnp.int32)
    cosine_table, sine_table = rope_tables(positions, HEAD)
    query_heads = queries.astype(jnp.float32).reshape(token_count, HEADS, HEAD)
    query_heads = rotate_pairs(head_norm(query_heads, query_gain.reshape(1, HEADS, HEAD)), cosine_table, sine_table)
    query_heads = lax.optimization_barrier(query_heads.astype(jnp.bfloat16))
    key_heads = keys.astype(jnp.float32).reshape(token_count, KV_HEADS, HEAD)
    key_heads = rotate_pairs(head_norm(key_heads, key_gain.reshape(1, 1, HEAD)), cosine_table, sine_table)
    key_wide = lax.optimization_barrier(key_heads.astype(jnp.bfloat16)).astype(jnp.float32)
    value_wide = values.astype(jnp.float32).reshape(token_count, KV_HEADS, HEAD)
    share = HEADS // KV_HEADS
    score_scale = HEAD ** (-0.5)
    query_blocks = query_heads.reshape(token_count // query_block, query_block, KV_HEADS, share, HEAD)

    def attend(block_queries):
        scores = jnp.einsum('qkgd,skd->kgqs', block_queries.astype(jnp.float32), key_wide) * score_scale
        row_max = lax.optimization_barrier(jnp.max(scores, axis=-1, keepdims=True))
        raised = jnp.exp(scores - row_max)
        row_total = lax.optimization_barrier(jnp.sum(raised, axis=-1))
        rounded = lax.optimization_barrier(raised.astype(jnp.bfloat16)).astype(jnp.float32)
        summed = jnp.einsum('kgqs,skd->qkgd', rounded, value_wide)
        return summed / jnp.transpose(row_total, (2, 0, 1))[..., None]
    attended = lax.map(attend, query_blocks).reshape(token_count, HEADS * HEAD).astype(jnp.bfloat16)
    update = jnp.dot(attended, out_weight, preferred_element_type=jnp.float32)
    updated = lax.optimization_barrier((residual.astype(jnp.float32) + update).astype(jnp.bfloat16))
    updated_wide = updated.astype(jnp.float32)
    normed = (updated_wide * lax.rsqrt(lax.optimization_barrier(jnp.mean(updated_wide * updated_wide, axis=1, keepdims=True)) + norm_eps) * norm_gain[None, :]).astype(jnp.bfloat16)
    mixing = group_prob[:, None] * jax.nn.softmax(expert_scores, axis=1)
    chosen_flat = route_experts.reshape(-1).astype(jnp.int32)
    owner = (jnp.arange(chosen_flat.shape[0], dtype=jnp.int32) // TOP).astype(jnp.int32)
    mixing_flat = mixing.reshape(-1)
    slot_limit = CAP * N_SP * N_TP
    block_count = EXPERT_HIDDEN // UNIT_BLOCK

    def one_expert(combined, inputs):
        gate_matrix, up_matrix, down_matrix, expert_id = inputs
        chosen = chosen_flat == expert_id
        ordinal = jnp.cumsum(chosen.astype(jnp.int32)) - 1
        target = jnp.where(chosen, ordinal, slot_limit).astype(jnp.int32)
        members = jnp.zeros((slot_limit,), jnp.int32).at[target].set(owner, mode='drop')
        member_weight = jnp.zeros((slot_limit,), jnp.float32).at[target].set(mixing_flat, mode='drop')
        picked = normed[members]
        gate_part = jnp.dot(picked, gate_matrix, preferred_element_type=jnp.float32)
        up_part = jnp.dot(picked, up_matrix, preferred_element_type=jnp.float32)
        hidden = lax.optimization_barrier((jax.nn.silu(gate_part) * up_part).astype(jnp.bfloat16))
        hidden_blocks = hidden.astype(jnp.float32).reshape(slot_limit, block_count, UNIT_BLOCK)
        down_blocks = down_matrix.astype(jnp.float32).reshape(block_count, UNIT_BLOCK, D)
        partial_value = jnp.einsum('rbh,bhd->rbd', hidden_blocks, down_blocks)
        rounded = lax.optimization_barrier(partial_value.astype(jnp.bfloat16)).astype(jnp.float32)
        expert_out = lax.optimization_barrier(lax.optimization_barrier(jnp.sum(rounded, axis=1)).astype(jnp.bfloat16))
        combined = combined.at[members].add(member_weight[:, None] * expert_out.astype(jnp.float32))
        return (combined, None)
    combined, unused = lax.scan(one_expert, jnp.zeros((token_count, D), jnp.float32), (w_gate, w_up, w_down, jnp.arange(EXPERTS, dtype=jnp.int32)))
    return (updated_wide + combined).astype(jnp.bfloat16)
```

```python
import functools

import jax
import jax.numpy as jnp
from jax import lax
from jax.experimental import pallas as pl
from jax.experimental.pallas import tpu as pltpu
from jax.sharding import PartitionSpec as P


GROUPS = 2
GRID_W = 64

rope_base = 10000.0
norm_eps = 1e-06
LOG2E = 1.4426950408889634


def rope_tables(first_token, span_tokens, head_size):
    lane = jnp.arange(head_size, dtype=jnp.int32)
    half, quarter = head_size // 2, head_size // 4
    index = (lane // 2) % quarter
    frequency = rope_base ** (-index.astype(jnp.float32) * 4.0 / head_size)
    sign = jnp.where(lane % 2 == 0, -1.0, 1.0).astype(jnp.float32)
    rows = (first_token // GRID_W + jnp.arange(span_tokens // GRID_W, dtype=jnp.int32)).astype(
        jnp.float32
    )
    columns = jnp.arange(GRID_W, dtype=jnp.float32)
    angles = jnp.concatenate([rows, columns])[:, None] * frequency[None, :]
    cosines, sines = lax.optimization_barrier((jnp.cos(angles), jnp.sin(angles) * sign[None, :]))

    def spread(table):
        row_part = table[: rows.shape[0]][:, None, :]
        column_part = table[rows.shape[0] :][None, :, :]
        return jnp.where(lane[None, None, :] < half, row_part, column_part).reshape(
            span_tokens, head_size
        )

    return spread(cosines), spread(sines)


def norm_turn(raw, gain, cosines, sines):
    wide = raw.astype(jnp.float32)
    size = wide.shape[1]
    factor = lax.rsqrt(jnp.mean(wide * wide, axis=1, keepdims=True) + norm_eps)
    scaled = wide * factor * gain
    lane = lax.broadcasted_iota(jnp.int32, scaled.shape, 1)
    swapped = jnp.where(
        lane % 2 == 0, pltpu.roll(scaled, size - 1, 1), pltpu.roll(scaled, 1, 1)
    )
    return (scaled * cosines + swapped * sines).astype(jnp.bfloat16)


def prep_kernel(place_ref, key_ref, value_ref, cos_ref, sin_ref, gain_ref, out_ref):
    size = key_ref.shape[1]
    out_ref[:, :size] = norm_turn(key_ref[...], gain_ref[...], cos_ref[...], sin_ref[...])
    out_ref[:, size:] = value_ref[...]


def prep_keys(keys, values, key_gain, cosines, sines, place, parts):
    size = cosines.shape[1]
    span = cosines.shape[0] // parts
    block = min(span, 512)
    steps = span // block
    spec = pltpu.PrefetchScalarGridSpec(
        num_scalar_prefetch=1,
        grid=(steps,),
        in_specs=[
            pl.BlockSpec((block, size), lambda i, h: (i + h[1] * steps, h[0])),
            pl.BlockSpec((block, size), lambda i, h: (i + h[1] * steps, h[0])),
            pl.BlockSpec((block, size), lambda i, h: (i + h[1] * steps, 0)),
            pl.BlockSpec((block, size), lambda i, h: (i + h[1] * steps, 0)),
            pl.BlockSpec((1, size), lambda i, h: (0, 0)),
        ],
        out_specs=pl.BlockSpec((block, 2 * size), lambda i, h: (i, 0)),
    )
    return pl.pallas_call(
        prep_kernel,
        grid_spec=spec,
        out_shape=jax.ShapeDtypeStruct((span, 2 * size), jnp.bfloat16),
        cost_estimate=pl.CostEstimate(flops=span * size * 16, bytes_accessed=span * size * 16, transcendentals=0),
        name="prep_keys",
    )(place, keys, values, cosines, sines, key_gain.reshape(1, size))


def attend_kernel(count, chunk, q_ref, cos_ref, sin_ref, gain_ref, *rest):
    kv_refs, out_ref, wide_values = rest[:count], rest[count], rest[count + 1]
    size = q_ref.shape[1]
    span = kv_refs[0].shape[0]

    @pl.when((pl.program_id(0) == 0) & (pl.program_id(1) == 0))
    def _():
        for n, kv in enumerate(kv_refs):
            wide_values[n * span : (n + 1) * span, :size] = kv[:, size:]
        wide_values[:, size:] = jnp.ones((wide_values.shape[0], size), jnp.bfloat16)

    query = norm_turn(q_ref[...], gain_ref[...], cos_ref[...], sin_ref[...])
    scores = []
    for kv in kv_refs:
        for start in range(0, span, chunk):
            scores.append(
                lax.dot_general(
                    query,
                    kv[start : start + chunk, :size],
                    (((1,), (1,)), ((), ())),
                    preferred_element_type=jnp.float32,
                )
            )
    top = functools.reduce(jnp.maximum, [jnp.max(s, axis=1, keepdims=True) for s in scores])
    factor = size ** (-0.5) * LOG2E
    total = None
    for n, s in enumerate(scores):
        raised = jnp.exp2((s - top) * factor).astype(jnp.bfloat16)
        part = jnp.dot(
            raised,
            wide_values[n * chunk : (n + 1) * chunk, :],
            preferred_element_type=jnp.float32,
        )
        total = part if total is None else total + part
    out_ref[...] = (total[:, :size] / total[:, size:]).astype(jnp.bfloat16)


def attend(queries, query_gain, cosines, sines, pieces):
    span, size = cosines.shape
    local_heads = queries.shape[1] // size
    piece_rows = pieces[0].shape[0]
    key_total = piece_rows * len(pieces)
    block = min(span, max(8, (1 << 20) // key_total))
    chunk = min(piece_rows, 1024)
    whole = pl.BlockSpec((piece_rows, 2 * size), lambda h, i: (0, 0))
    return pl.pallas_call(
        functools.partial(attend_kernel, len(pieces), chunk),
        grid=(local_heads, span // block),
        in_specs=[
            pl.BlockSpec((block, size), lambda h, i: (i, h)),
            pl.BlockSpec((block, size), lambda h, i: (i, 0)),
            pl.BlockSpec((block, size), lambda h, i: (i, 0)),
            pl.BlockSpec((1, size), lambda h, i: (0, h)),
        ]
        + [whole] * len(pieces),
        out_specs=pl.BlockSpec((block, size), lambda h, i: (i, h)),
        out_shape=jax.ShapeDtypeStruct(queries.shape, jnp.bfloat16),
        scratch_shapes=[pltpu.VMEM((key_total, 2 * size), jnp.bfloat16)],
        compiler_params=pltpu.CompilerParams(vmem_limit_bytes=56 * 1024 * 1024),
        cost_estimate=pl.CostEstimate(
            flops=8 * span * local_heads * key_total * size,
            bytes_accessed=4 * key_total * size * 2,
            transcendentals=span * local_heads * key_total,
        ),
        name="attend",
    )(queries, cosines, sines, query_gain.reshape(1, -1), *pieces)


def routed_general(normed, route_experts, w_gate, w_up, w_down, mixing):
    row_count, model_width = normed.shape
    seq_size = lax.axis_size("sp")
    local_experts = w_gate.shape[0]
    expert_total = local_experts * seq_size
    group_experts = expert_total // GROUPS
    top_count = route_experts.shape[1]
    capacity = (top_count * (5 * row_count // 8) + group_experts - 1) // group_experts
    chosen_flat = route_experts.reshape(-1)
    expert_ids = jnp.arange(expert_total, dtype=jnp.int32)
    onehot = (chosen_flat[:, None] == expert_ids[None, :]).astype(jnp.int32)
    ordinal = jnp.sum((jnp.cumsum(onehot, axis=0) - onehot) * onehot, axis=1)
    slot_of = chosen_flat * capacity + ordinal
    slot_ids = jnp.arange(expert_total * capacity, dtype=jnp.int32)
    placing = jnp.any(
        slot_ids[:, None, None] == slot_of.reshape(row_count, top_count)[None, :, :], axis=2
    ).astype(jnp.bfloat16)
    full_down = lax.all_gather(w_down, "tp", axis=1, tiled=True)
    outgoing = jnp.dot(placing, normed, preferred_element_type=jnp.float32).astype(jnp.bfloat16)
    outgoing = outgoing.reshape(seq_size, local_experts, capacity, model_width)
    arrived = lax.all_to_all(outgoing, "sp", split_axis=0, concat_axis=0, tiled=True)
    piece = lax.all_gather(arrived, "tp", axis=0, tiled=True)
    gate_part = jnp.einsum("secd,edh->sech", piece, w_gate, preferred_element_type=jnp.float32)
    up_part = jnp.einsum("secd,edh->sech", piece, w_up, preferred_element_type=jnp.float32)
    hidden = (jax.nn.silu(gate_part) * up_part).astype(jnp.bfloat16)
    unit_rows = lax.all_to_all(hidden, "tp", split_axis=0, concat_axis=3, tiled=True)
    returned = jnp.einsum(
        "sech,ehd->secd", unit_rows, full_down, preferred_element_type=jnp.float32
    ).astype(jnp.bfloat16)
    result_rows = lax.all_to_all(returned, "sp", split_axis=0, concat_axis=0, tiled=True).reshape(
        expert_total * capacity, model_width
    )
    picked = result_rows[slot_of].astype(jnp.float32).reshape(row_count, top_count, model_width)
    return jnp.sum(picked * mixing[:, :, None], axis=1)


def swap(array, bits, tp_bits=0):
    count, width = lax.axis_size("sp"), lax.axis_size("tp")
    if tp_bits == 0:
        return lax.ppermute(array, "sp", [(s, s ^ bits) for s in range(count)])
    if bits == 0:
        return lax.ppermute(array, "tp", [(t, t ^ tp_bits) for t in range(width)])
    pairs = [
        (s * width + t, (s ^ bits) * width + (t ^ tp_bits))
        for s in range(count)
        for t in range(width)
    ]
    return lax.ppermute(array, ("sp", "tp"), pairs)


def mesh_peer(seq_bits, model_bits):
    return {"sp": lax.axis_index("sp") ^ seq_bits, "tp": lax.axis_index("tp") ^ model_bits}


def expert_kernel(
    own_ref,
    gate_ref,
    up_ref,
    down_ref,
    gate_far_ref,
    up_far_ref,
    down_far_ref,
    out_ref,
    gates,
    ups,
    downs,
    rows,
    total,
    kept,
    parts,
    landed,
    load_sems,
    weight_send,
    weight_recv,
    row_send,
    row_recv,
    part_send,
    part_recv,
):
    capacity, width = out_ref.shape[0] // 2, out_ref.shape[1]
    parity = lax.axis_index("sp") % 2
    across_y, across_x = mesh_peer(2, 0), mesh_peer(1, 0)
    across_z, sibling = mesh_peer(0, 4), mesh_peer(0, 1)

    barrier = pltpu.get_barrier_semaphore()
    for peer in (across_y, across_x, across_z, sibling):
        pl.semaphore_signal(
            barrier, inc=1, device_id=peer, device_id_type=pl.DeviceIdType.MESH
        )
    pl.semaphore_wait(barrier, 4)

    def remote(source, target, send, recv, peer):
        copy = pltpu.make_async_remote_copy(
            src_ref=source,
            dst_ref=target,
            send_sem=send,
            recv_sem=recv,
            device_id=peer,
            device_id_type=pl.DeviceIdType.MESH,
        )
        copy.start()
        return copy

    def send_rows(n, source, slot, peer):
        return remote(source, rows.at[slot], row_send.at[n], row_recv.at[slot], peer)

    def send_part(n, peer):
        return remote(parts.at[n], landed.at[n], part_send.at[n], part_recv.at[n], peer)

    sent = [
        send_rows(0, own_ref.at[1], 1, across_y),
        send_rows(1, own_ref.at[0], 2, across_x),
        send_rows(2, own_ref.at[0], 4, across_z),
    ]
    arriving = {1: sent[0], 2: sent[1], 4: sent[2]}

    weights = []
    loads = []
    holders = ((gate_ref, gates), (up_ref, ups), (down_ref, downs))
    far_holders = ((gate_far_ref, gates), (up_far_ref, ups), (down_far_ref, downs))
    for block, group in ((0, holders), (2, far_holders)):
        for n, (source, target) in enumerate(group):
            k = block // 2 * 3 + n
            load = pltpu.make_async_copy(source, target.at[block], load_sems.at[k])
            load.start()
            loads.append(load)
            weights.append(
                remote(source, target.at[block + 1], weight_send.at[k], weight_recv.at[k], sibling)
            )

    def ffn(tokens):
        mix = tokens[:, width : width + 128].astype(jnp.float32)
        scale = jnp.where(
            parity == 0, mix[:, 0:1] + mix[:, 1:2], mix[:, 2:3] + mix[:, 3:4]
        )

        def step(block, carry):
            gate_part = jnp.dot(
                tokens[:, :width], gates[block], preferred_element_type=jnp.float32
            )
            up_part = jnp.dot(tokens[:, :width], ups[block], preferred_element_type=jnp.float32)
            hidden = (gate_part / (1.0 + jnp.exp(-gate_part)) * up_part * scale).astype(
                jnp.bfloat16
            )
            part = jnp.dot(hidden, downs[block], preferred_element_type=jnp.float32)

            @pl.when(block == 0)
            def _():
                total[...] = part

            @pl.when(block > 0)
            def _():
                total[...] += part

            return carry

        lax.fori_loop(0, gates.shape[0], step, 0)

    def part_of(n, slot, peer):
        ffn(rows.at[slot])
        parts[n] = total[...].astype(jnp.bfloat16)
        return send_part(n, peer)

    arriving[1].wait_recv()
    second = [
        send_rows(3, rows.at[1], 3, across_x),
        send_rows(4, rows.at[1], 5, across_z),
    ]
    for load in loads:
        load.wait()
    for weight in weights:
        weight.wait_recv()
    arriving[2].wait_recv()
    exchanges = [part_of(0, 2, across_x)]
    arriving[4].wait_recv()
    third = send_rows(5, rows.at[4], 6, across_x)
    ffn(rows.at[4])
    kept[2] = total[...]
    second[0].wait_recv()
    exchanges.append(part_of(1, 3, across_x))
    ffn(own_ref.at[0])
    kept[0] = total[...]
    third.wait_recv()
    exchanges.append(part_of(2, 6, across_x))
    second[1].wait_recv()
    fourth = send_rows(6, rows.at[5], 7, across_x)
    ffn(rows.at[5])
    kept[3] = total[...]
    exchanges[2].wait_recv()
    parts[4] = (kept[2] + landed[2].astype(jnp.float32)).astype(jnp.bfloat16)
    hops = [send_part(4, across_z)]
    fourth.wait_recv()
    exchanges.append(part_of(3, 7, across_x))
    ffn(rows.at[1])
    kept[1] = total[...]
    exchanges[3].wait_recv()
    parts[5] = (kept[3] + landed[3].astype(jnp.float32)).astype(jnp.bfloat16)
    hops.append(send_part(5, across_z))
    exchanges[0].wait_recv()
    hops[0].wait_recv()
    out_ref[:capacity, :] = (
        kept[0] + landed[0].astype(jnp.float32) + landed[4].astype(jnp.float32)
    ).astype(jnp.bfloat16)
    exchanges[1].wait_recv()
    hops[1].wait_recv()
    parts[6] = (
        kept[1] + landed[1].astype(jnp.float32) + landed[5].astype(jnp.float32)
    ).astype(jnp.bfloat16)
    back = send_part(6, across_y)
    back.wait_recv()
    out_ref[capacity:, :] = landed[6]
    for copy in sent + second + [third, fourth] + weights + exchanges + hops + [back]:
        copy.wait_send()


def run_experts(own, near, far):
    half, capacity, wide = own.shape
    width, units = near[0].shape
    blocks = 4
    flops = 2 * 8 * capacity * blocks * units * width * 3
    whole = pl.BlockSpec(memory_space=pltpu.VMEM)
    distant = pl.BlockSpec(memory_space=pl.ANY)
    return pl.pallas_call(
        expert_kernel,
        out_shape=jax.ShapeDtypeStruct((half * capacity, width), jnp.bfloat16),
        in_specs=[whole] + [distant] * 6,
        out_specs=whole,
        scratch_shapes=[
            pltpu.VMEM((blocks, width, units), jnp.bfloat16),
            pltpu.VMEM((blocks, width, units), jnp.bfloat16),
            pltpu.VMEM((blocks, units, width), jnp.bfloat16),
            pltpu.VMEM((8, capacity, wide), jnp.bfloat16),
            pltpu.VMEM((capacity, width), jnp.float32),
            pltpu.VMEM((4, capacity, width), jnp.float32),
            pltpu.VMEM((7, capacity, width), jnp.bfloat16),
            pltpu.VMEM((7, capacity, width), jnp.bfloat16),
            pltpu.SemaphoreType.DMA((6,)),
            pltpu.SemaphoreType.DMA((6,)),
            pltpu.SemaphoreType.DMA((6,)),
            pltpu.SemaphoreType.DMA((7,)),
            pltpu.SemaphoreType.DMA((8,)),
            pltpu.SemaphoreType.DMA((7,)),
            pltpu.SemaphoreType.DMA((7,)),
        ],
        compiler_params=pltpu.CompilerParams(
            collective_id=1, has_side_effects=True, vmem_limit_bytes=48 * 1024 * 1024
        ),
        cost_estimate=pl.CostEstimate(
            flops=flops, bytes_accessed=12 * width * units * 2, transcendentals=0
        ),
        name="experts",
    )(own, *near, *far)


def routed_pairs(normed, route_experts, near, far, mixing):
    row_count, width = normed.shape
    me = lax.axis_index("sp")
    capacity = 5 * row_count // 8
    held = 2 * capacity
    group = route_experts[:, 0] // 2
    token = jnp.arange(row_count, dtype=jnp.int32)
    earlier = (group[:, None] == group[None, :]) & (token[None, :] < token[:, None])
    ordinal = jnp.sum(earlier.astype(jnp.int32), axis=1)
    slot = jnp.where(group == me // 2, 0, capacity) + ordinal
    slot_ids = jnp.arange(held, dtype=jnp.int32)
    placing = (slot_ids[:, None] == slot[None, :]).astype(jnp.bfloat16)
    shares = jnp.stack(
        [jnp.sum(jnp.where(route_experts % 2 == p, mixing, 0.0), axis=1) for p in (0, 1)], axis=1
    )
    coarse = lax.reduce_precision(shares, 8, 7)
    lane = jnp.arange(128, dtype=jnp.int32)[None, :]
    extra = jnp.zeros((row_count, 128), jnp.float32)
    for p in (0, 1):
        extra = jnp.where(lane == 2 * p, coarse[:, p : p + 1], extra)
        extra = jnp.where(lane == 2 * p + 1, (shares - coarse)[:, p : p + 1], extra)
    extended = jnp.concatenate([normed, extra.astype(jnp.bfloat16)], axis=1)
    own = jnp.dot(placing, extended, preferred_element_type=jnp.float32).astype(jnp.bfloat16)
    results = run_experts(own.reshape(2, capacity, width + 128), near, far)
    return lax.dot_general(
        placing, results, (((0,), (0,)), ((), ())), preferred_element_type=jnp.float32
    )


def local(
    queries,
    keys,
    values,
    query_gain,
    key_gain,
    out_weight,
    residual,
    norm_gain,
    route_experts,
    expert_scores,
    group_prob,
    w_gate,
    w_up,
    w_down,
):
    span_tokens = queries.shape[0]
    head_size = key_gain.shape[0]
    local_heads = queries.shape[1] // head_size
    key_heads = keys.shape[1] // head_size
    model_size = lax.axis_size("tp")
    seq_size = lax.axis_size("sp")
    share = local_heads * model_size // key_heads
    model_index = lax.axis_index("tp")
    seq_index = lax.axis_index("sp")
    local_experts = w_gate.shape[0]
    group_experts = local_experts * seq_size // GROUPS
    pairs = (
        local_experts == 1
        and GROUPS == 2
        and group_experts == 2
        and route_experts.shape[1] == 2
        and model_size == 8
    )
    halves = seq_size == 4 and model_size % 2 == 0 and share % (2 * local_heads) == 0

    cosines, sines = rope_tables(seq_index * span_tokens, span_tokens, head_size)
    shared_head = (model_index * local_heads // share).astype(jnp.int32)
    core = (model_index % 2 if halves else 0 * model_index).astype(jnp.int32)
    key_values = prep_keys(
        keys, values, key_gain, cosines, sines, jnp.stack([shared_head, core]), 2 if halves else 1
    )
    if halves:
        fetched = [key_values]
        for bits in (1, 2, 3):
            fetched.append(swap(key_values, bits))
        pieces = fetched + [swap(piece, 0, 1) for piece in fetched]
    else:
        pieces = [lax.all_gather(key_values, "sp", axis=0, tiled=True)]
    if pairs:
        near = (w_gate[0], w_up[0], w_down[0])
        far = []
        for block in near:
            far.append(swap(block, 0, 2))
    attended = attend(queries, query_gain, cosines, sines, pieces)
    all_heads = lax.all_to_all(attended, "tp", split_axis=0, concat_axis=1, tiled=True)
    update = jnp.dot(all_heads, out_weight, preferred_element_type=jnp.float32)
    updated = lax.optimization_barrier((residual.astype(jnp.float32) + update).astype(jnp.bfloat16))
    updated_wide = updated.astype(jnp.float32)
    normed = (
        updated_wide
        * lax.rsqrt(jnp.mean(updated_wide * updated_wide, axis=1, keepdims=True) + norm_eps)
        * norm_gain[None, :]
    ).astype(jnp.bfloat16)
    mixing = group_prob[:, None] * jax.nn.softmax(expert_scores, axis=1)
    if pairs:
        combined = routed_pairs(normed, route_experts, near, far, mixing)
    else:
        combined = routed_general(normed, route_experts, w_gate, w_up, w_down, mixing)
    return (updated_wide + combined).astype(jnp.bfloat16)


def solution(mesh):
    placed = (
        P("sp", "tp"),
        P("sp", None),
        P("sp", None),
        P("tp"),
        P(),
        P(),
        P(("sp", "tp"), None),
        P(),
        P(("sp", "tp"), None),
        P(("sp", "tp"), None),
        P(("sp", "tp")),
        P("sp", None, "tp"),
        P("sp", None, "tp"),
        P("sp", "tp", None),
    )
    return jax.shard_map(
        local, mesh=mesh, in_specs=placed, out_specs=P(("sp", "tp"), None), check_vma=False
    )
```

```python
import functools

import jax
import jax.numpy as jnp
from jax import lax
from jax.experimental import pallas as pl
from jax.experimental.pallas import tpu as pltpu
from jax.sharding import PartitionSpec as P


GROUPS = 2
GRID_W = 64

rope_base = 10000.0
norm_eps = 1e-06
LOG2E = 1.4426950408889634


def rope_tables(first_token, span_tokens, head_size):
    lane = jnp.arange(head_size, dtype=jnp.int32)
    half, quarter = head_size // 2, head_size // 4
    index = (lane // 2) % quarter
    frequency = rope_base ** (-index.astype(jnp.float32) * 4.0 / head_size)
    sign = jnp.where(lane % 2 == 0, -1.0, 1.0).astype(jnp.float32)
    rows = (first_token // GRID_W + jnp.arange(span_tokens // GRID_W, dtype=jnp.int32)).astype(
        jnp.float32
    )
    columns = jnp.arange(GRID_W, dtype=jnp.float32)
    angles = jnp.concatenate([rows, columns])[:, None] * frequency[None, :]
    cosines, sines = lax.optimization_barrier((jnp.cos(angles), jnp.sin(angles) * sign[None, :]))

    def spread(table):
        row_part = table[: rows.shape[0]][:, None, :]
        column_part = table[rows.shape[0] :][None, :, :]
        return jnp.where(lane[None, None, :] < half, row_part, column_part).reshape(
            span_tokens, head_size
        )

    return spread(cosines), spread(sines)


def norm_turn(raw, gain, cosines, sines):
    wide = raw.astype(jnp.float32)
    size = wide.shape[1]
    factor = lax.rsqrt(jnp.mean(wide * wide, axis=1, keepdims=True) + norm_eps)
    scaled = wide * factor * gain
    lane = lax.broadcasted_iota(jnp.int32, scaled.shape, 1)
    swapped = jnp.where(
        lane % 2 == 0, pltpu.roll(scaled, size - 1, 1), pltpu.roll(scaled, 1, 1)
    )
    return (scaled * cosines + swapped * sines).astype(jnp.bfloat16)


def prep_kernel(place_ref, key_ref, value_ref, cos_ref, sin_ref, gain_ref, out_ref):
    size = key_ref.shape[1]
    out_ref[:, :size] = norm_turn(key_ref[...], gain_ref[...], cos_ref[...], sin_ref[...])
    out_ref[:, size:] = value_ref[...]


def prep_keys(keys, values, key_gain, cosines, sines, place, parts):
    size = cosines.shape[1]
    span = cosines.shape[0] // parts
    block = min(span, 512)
    steps = span // block
    spec = pltpu.PrefetchScalarGridSpec(
        num_scalar_prefetch=1,
        grid=(steps,),
        in_specs=[
            pl.BlockSpec((block, size), lambda i, h: (i + h[1] * steps, h[0])),
            pl.BlockSpec((block, size), lambda i, h: (i + h[1] * steps, h[0])),
            pl.BlockSpec((block, size), lambda i, h: (i + h[1] * steps, 0)),
            pl.BlockSpec((block, size), lambda i, h: (i + h[1] * steps, 0)),
            pl.BlockSpec((1, size), lambda i, h: (0, 0)),
        ],
        out_specs=pl.BlockSpec((block, 2 * size), lambda i, h: (i, 0)),
    )
    return pl.pallas_call(
        prep_kernel,
        grid_spec=spec,
        out_shape=jax.ShapeDtypeStruct((span, 2 * size), jnp.bfloat16),
        cost_estimate=pl.CostEstimate(flops=span * size * 16, bytes_accessed=span * size * 16, transcendentals=0),
        name="prep_keys",
    )(place, keys, values, cosines, sines, key_gain.reshape(1, size))


def attend_kernel(count, chunk, q_ref, cos_ref, sin_ref, gain_ref, *rest):
    kv_refs, out_ref, wide_values = rest[:count], rest[count], rest[count + 1]
    size = q_ref.shape[1]
    span = kv_refs[0].shape[0]

    @pl.when((pl.program_id(0) == 0) & (pl.program_id(1) == 0))
    def _():
        for n, kv in enumerate(kv_refs):
            wide_values[n * span : (n + 1) * span, :size] = kv[:, size:]
        wide_values[:, size:] = jnp.ones((wide_values.shape[0], size), jnp.bfloat16)

    query = norm_turn(q_ref[...], gain_ref[...], cos_ref[...], sin_ref[...])
    scores = []
    for kv in kv_refs:
        for start in range(0, span, chunk):
            scores.append(
                lax.dot_general(
                    query,
                    kv[start : start + chunk, :size],
                    (((1,), (1,)), ((), ())),
                    preferred_element_type=jnp.float32,
                )
            )
    top = functools.reduce(jnp.maximum, [jnp.max(s, axis=1, keepdims=True) for s in scores])
    factor = size ** (-0.5) * LOG2E
    total = None
    for n, s in enumerate(scores):
        raised = jnp.exp2((s - top) * factor).astype(jnp.bfloat16)
        part = jnp.dot(
            raised,
            wide_values[n * chunk : (n + 1) * chunk, :],
            preferred_element_type=jnp.float32,
        )
        total = part if total is None else total + part
    out_ref[...] = (total[:, :size] / total[:, size:]).astype(jnp.bfloat16)


def attend(queries, query_gain, cosines, sines, pieces):
    span, size = cosines.shape
    local_heads = queries.shape[1] // size
    piece_rows = pieces[0].shape[0]
    key_total = piece_rows * len(pieces)
    block = min(span, max(8, (1 << 20) // key_total))
    chunk = min(piece_rows, 1024)
    whole = pl.BlockSpec((piece_rows, 2 * size), lambda h, i: (0, 0))
    return pl.pallas_call(
        functools.partial(attend_kernel, len(pieces), chunk),
        grid=(local_heads, span // block),
        in_specs=[
            pl.BlockSpec((block, size), lambda h, i: (i, h)),
            pl.BlockSpec((block, size), lambda h, i: (i, 0)),
            pl.BlockSpec((block, size), lambda h, i: (i, 0)),
            pl.BlockSpec((1, size), lambda h, i: (0, h)),
        ]
        + [whole] * len(pieces),
        out_specs=pl.BlockSpec((block, size), lambda h, i: (i, h)),
        out_shape=jax.ShapeDtypeStruct(queries.shape, jnp.bfloat16),
        scratch_shapes=[pltpu.VMEM((key_total, 2 * size), jnp.bfloat16)],
        compiler_params=pltpu.CompilerParams(vmem_limit_bytes=56 * 1024 * 1024),
        cost_estimate=pl.CostEstimate(
            flops=8 * span * local_heads * key_total * size,
            bytes_accessed=4 * key_total * size * 2,
            transcendentals=span * local_heads * key_total,
        ),
        name="attend",
    )(queries, cosines, sines, query_gain.reshape(1, -1), *pieces)


def routed_general(normed, route_experts, w_gate, w_up, w_down, mixing):
    row_count, model_width = normed.shape
    seq_size = lax.axis_size("sp")
    local_experts = w_gate.shape[0]
    expert_total = local_experts * seq_size
    group_experts = expert_total // GROUPS
    top_count = route_experts.shape[1]
    capacity = (top_count * (5 * row_count // 8) + group_experts - 1) // group_experts
    chosen_flat = route_experts.reshape(-1)
    expert_ids = jnp.arange(expert_total, dtype=jnp.int32)
    onehot = (chosen_flat[:, None] == expert_ids[None, :]).astype(jnp.int32)
    ordinal = jnp.sum((jnp.cumsum(onehot, axis=0) - onehot) * onehot, axis=1)
    slot_of = chosen_flat * capacity + ordinal
    slot_ids = jnp.arange(expert_total * capacity, dtype=jnp.int32)
    placing = jnp.any(
        slot_ids[:, None, None] == slot_of.reshape(row_count, top_count)[None, :, :], axis=2
    ).astype(jnp.bfloat16)
    full_down = lax.all_gather(w_down, "tp", axis=1, tiled=True)
    outgoing = jnp.dot(placing, normed, preferred_element_type=jnp.float32).astype(jnp.bfloat16)
    outgoing = outgoing.reshape(seq_size, local_experts, capacity, model_width)
    arrived = lax.all_to_all(outgoing, "sp", split_axis=0, concat_axis=0, tiled=True)
    piece = lax.all_gather(arrived, "tp", axis=0, tiled=True)
    gate_part = jnp.einsum("secd,edh->sech", piece, w_gate, preferred_element_type=jnp.float32)
    up_part = jnp.einsum("secd,edh->sech", piece, w_up, preferred_element_type=jnp.float32)
    hidden = (jax.nn.silu(gate_part) * up_part).astype(jnp.bfloat16)
    unit_rows = lax.all_to_all(hidden, "tp", split_axis=0, concat_axis=3, tiled=True)
    returned = jnp.einsum(
        "sech,ehd->secd", unit_rows, full_down, preferred_element_type=jnp.float32
    ).astype(jnp.bfloat16)
    result_rows = lax.all_to_all(returned, "sp", split_axis=0, concat_axis=0, tiled=True).reshape(
        expert_total * capacity, model_width
    )
    picked = result_rows[slot_of].astype(jnp.float32).reshape(row_count, top_count, model_width)
    return jnp.sum(picked * mixing[:, :, None], axis=1)


def swap(array, bits, tp_bits=0):
    count, width = lax.axis_size("sp"), lax.axis_size("tp")
    if tp_bits == 0:
        return lax.ppermute(array, "sp", [(s, s ^ bits) for s in range(count)])
    if bits == 0:
        return lax.ppermute(array, "tp", [(t, t ^ tp_bits) for t in range(width)])
    pairs = [
        (s * width + t, (s ^ bits) * width + (t ^ tp_bits))
        for s in range(count)
        for t in range(width)
    ]
    return lax.ppermute(array, ("sp", "tp"), pairs)


def mesh_peer(seq_bits, model_bits):
    return {"sp": lax.axis_index("sp") ^ seq_bits, "tp": lax.axis_index("tp") ^ model_bits}


def expert_kernel(
    own_ref,
    gate_ref,
    up_ref,
    down_ref,
    gate_far_ref,
    up_far_ref,
    down_far_ref,
    out_ref,
    gates,
    ups,
    downs,
    rows,
    hidden,
    kept,
    parts,
    landed,
    load_sems,
    weight_send,
    weight_recv,
    row_send,
    row_recv,
    part_send,
    part_recv,
):
    capacity, width = out_ref.shape[0] // 2, out_ref.shape[1]
    units = gate_ref.shape[1]
    blocks = gates.shape[0]
    first = (capacity // 2 + 15) // 16 * 16
    pieces = (pl.ds(0, first), pl.ds(first, capacity - first))
    full = pl.ds(0, capacity)
    parity = lax.axis_index("sp") % 2
    across_y, across_x = mesh_peer(2, 0), mesh_peer(1, 0)
    across_z, sibling = mesh_peer(0, 4), mesh_peer(0, 1)

    barrier = pltpu.get_barrier_semaphore()
    for peer in (across_y, across_x, across_z, sibling):
        pl.semaphore_signal(
            barrier, inc=1, device_id=peer, device_id_type=pl.DeviceIdType.MESH
        )
    pl.semaphore_wait(barrier, 4)

    started = []

    def remote(source, target, send, recv, peer):
        copy = pltpu.make_async_remote_copy(
            src_ref=source,
            dst_ref=target,
            send_sem=send,
            recv_sem=recv,
            device_id=peer,
            device_id_type=pl.DeviceIdType.MESH,
        )
        copy.start()
        started.append(copy)
        return copy

    def send_rows(source, slot, p, span, peer):
        return remote(
            source.at[span],
            rows.at[slot, span],
            row_send.at[slot, p],
            row_recv.at[slot, p],
            peer,
        )

    def send_part(n, p, span, peer):
        return remote(
            parts.at[n, span],
            landed.at[n, span],
            part_send.at[n, p],
            part_recv.at[n, p],
            peer,
        )

    over_y = [send_rows(own_ref.at[1], 1, p, pieces[p], across_y) for p in (0, 1)]
    over_x = send_rows(own_ref.at[0], 2, 0, full, across_x)
    over_z = [send_rows(own_ref.at[0], 4, p, pieces[p], across_z) for p in (0, 1)]

    weights = []
    loads = []
    holders = ((gate_ref, gates), (up_ref, ups), (down_ref, downs))
    far_holders = ((gate_far_ref, gates), (up_far_ref, ups), (down_far_ref, downs))
    for block, group in ((0, holders), (2, far_holders)):
        for n, (source, target) in enumerate(group):
            k = block // 2 * 3 + n
            load = pltpu.make_async_copy(source, target.at[block], load_sems.at[k])
            load.start()
            loads.append(load)
            weights.append(
                remote(source, target.at[block + 1], weight_send.at[k], weight_recv.at[k], sibling)
            )

    def ffn(tokens, put):
        count = tokens.shape[0]
        mix = tokens[:, width : width + 128].astype(jnp.float32)
        scale = jnp.where(
            parity == 0, mix[:, 0:1] + mix[:, 1:2], mix[:, 2:3] + mix[:, 3:4]
        )
        for block in range(blocks):
            gate_part = jnp.dot(
                tokens[:, :width], gates[block], preferred_element_type=jnp.float32
            )
            up_part = jnp.dot(tokens[:, :width], ups[block], preferred_element_type=jnp.float32)
            hidden[:count, block * units : (block + 1) * units] = (
                gate_part / (1.0 + jnp.exp(-gate_part)) * up_part * scale
            ).astype(jnp.bfloat16)
        for start in range(0, width, 2 * units):
            columns = slice(start, start + 2 * units)
            total = None
            for block in range(blocks):
                part = jnp.dot(
                    hidden[:count, block * units : (block + 1) * units],
                    downs[block, :, columns],
                    preferred_element_type=jnp.float32,
                )
                total = part if total is None else total + part
            put(columns, total)

    def keep(n, tokens):
        def put(columns, total):
            kept[n, :, columns] = total

        ffn(tokens, put)

    def part_of(n, tokens, span):
        def put(columns, total):
            parts[n, span, columns] = total.astype(jnp.bfloat16)

        ffn(tokens, put)

    def hop(n, p):
        span = pieces[p]
        parts[4 + n, span] = (
            kept[2 + n, span] + landed[2 + n, span].astype(jnp.float32)
        ).astype(jnp.bfloat16)
        return send_part(4 + n, p, span, across_z)

    def settled(n, span):
        return (
            kept[n, span] + landed[n, span].astype(jnp.float32)
            + landed[4 + n, span].astype(jnp.float32)
        ).astype(jnp.bfloat16)

    over_x_far, over_z_far = [], []
    for p in (0, 1):
        over_y[p].wait_recv()
        over_x_far.append(send_rows(rows.at[1], 3, p, pieces[p], across_x))
        over_z_far.append(send_rows(rows.at[1], 5, p, pieces[p], across_z))
    over_z[0].wait_recv()
    passed = [send_rows(rows.at[4], 6, 0, pieces[0], across_x)]
    for load in loads:
        load.wait()
    for weight in weights:
        weight.wait_recv()
    keep(0, own_ref.at[0])
    over_z[1].wait_recv()
    passed.append(send_rows(rows.at[4], 6, 1, pieces[1], across_x))
    keep(2, rows.at[4])
    exchanged = []
    for p in (0, 1):
        passed[p].wait_recv()
        part_of(2, rows.at[6, pieces[p]], pieces[p])
        exchanged.append(send_part(2, p, pieces[p], across_x))
    over_z_far[0].wait_recv()
    passed_far = [send_rows(rows.at[5], 7, 0, pieces[0], across_x)]
    keep(1, rows.at[1])
    exchanged[0].wait_recv()
    hops = [hop(0, 0)]
    over_z_far[1].wait_recv()
    passed_far.append(send_rows(rows.at[5], 7, 1, pieces[1], across_x))
    keep(3, rows.at[5])
    passed_far[0].wait_recv()
    part_of(3, rows.at[7, pieces[0]], pieces[0])
    exchanged_far = [send_part(3, 0, pieces[0], across_x)]
    exchanged[1].wait_recv()
    hops.append(hop(0, 1))
    passed_far[1].wait_recv()
    part_of(3, rows.at[7, pieces[1]], pieces[1])
    exchanged_far.append(send_part(3, 1, pieces[1], across_x))
    exchanged_far[0].wait_recv()
    hops_far = [hop(1, 0)]
    for p in (0, 1):
        over_x_far[p].wait_recv()
    part_of(1, rows.at[3], full)
    direct_far = [send_part(1, p, pieces[p], across_x) for p in (0, 1)]
    exchanged_far[1].wait_recv()
    hops_far.append(hop(1, 1))
    over_x.wait_recv()
    part_of(0, rows.at[2], full)
    direct = send_part(0, 0, full, across_x)
    back = []
    for p in (0, 1):
        direct_far[p].wait_recv()
        hops_far[p].wait_recv()
        parts[6, pieces[p]] = settled(1, pieces[p])
        back.append(send_part(6, p, pieces[p], across_y))
    direct.wait_recv()
    for copy in hops:
        copy.wait_recv()
    out_ref[:capacity, :] = settled(0, full)
    for copy in back:
        copy.wait_recv()
    out_ref[capacity:, :] = landed[6]
    for copy in started:
        copy.wait_send()


def run_experts(own, near, far):
    half, capacity, wide = own.shape
    width, units = near[0].shape
    blocks = 4
    flops = 2 * 8 * capacity * blocks * units * width * 3
    whole = pl.BlockSpec(memory_space=pltpu.VMEM)
    distant = pl.BlockSpec(memory_space=pl.ANY)
    return pl.pallas_call(
        expert_kernel,
        out_shape=jax.ShapeDtypeStruct((half * capacity, width), jnp.bfloat16),
        in_specs=[whole] + [distant] * 6,
        out_specs=whole,
        scratch_shapes=[
            pltpu.VMEM((blocks, width, units), jnp.bfloat16),
            pltpu.VMEM((blocks, width, units), jnp.bfloat16),
            pltpu.VMEM((blocks, units, width), jnp.bfloat16),
            pltpu.VMEM((8, capacity, wide), jnp.bfloat16),
            pltpu.VMEM((capacity, blocks * units), jnp.bfloat16),
            pltpu.VMEM((4, capacity, width), jnp.float32),
            pltpu.VMEM((7, capacity, width), jnp.bfloat16),
            pltpu.VMEM((7, capacity, width), jnp.bfloat16),
            pltpu.SemaphoreType.DMA((6,)),
            pltpu.SemaphoreType.DMA((6,)),
            pltpu.SemaphoreType.DMA((6,)),
            pltpu.SemaphoreType.DMA((8, 2)),
            pltpu.SemaphoreType.DMA((8, 2)),
            pltpu.SemaphoreType.DMA((7, 2)),
            pltpu.SemaphoreType.DMA((7, 2)),
        ],
        compiler_params=pltpu.CompilerParams(
            collective_id=1, has_side_effects=True, vmem_limit_bytes=48 * 1024 * 1024
        ),
        cost_estimate=pl.CostEstimate(
            flops=flops, bytes_accessed=12 * width * units * 2, transcendentals=0
        ),
        name="experts",
    )(own, *near, *far)


def routed_pairs(normed, route_experts, near, far, mixing):
    row_count, width = normed.shape
    me = lax.axis_index("sp")
    capacity = 5 * row_count // 8
    held = 2 * capacity
    group = route_experts[:, 0] // 2
    token = jnp.arange(row_count, dtype=jnp.int32)
    earlier = (group[:, None] == group[None, :]) & (token[None, :] < token[:, None])
    ordinal = jnp.sum(earlier.astype(jnp.int32), axis=1)
    slot = jnp.where(group == me // 2, 0, capacity) + ordinal
    slot_ids = jnp.arange(held, dtype=jnp.int32)
    placing = (slot_ids[:, None] == slot[None, :]).astype(jnp.bfloat16)
    shares = jnp.stack(
        [jnp.sum(jnp.where(route_experts % 2 == p, mixing, 0.0), axis=1) for p in (0, 1)], axis=1
    )
    coarse = lax.reduce_precision(shares, 8, 7)
    lane = jnp.arange(128, dtype=jnp.int32)[None, :]
    extra = jnp.zeros((row_count, 128), jnp.float32)
    for p in (0, 1):
        extra = jnp.where(lane == 2 * p, coarse[:, p : p + 1], extra)
        extra = jnp.where(lane == 2 * p + 1, (shares - coarse)[:, p : p + 1], extra)
    extended = jnp.concatenate([normed, extra.astype(jnp.bfloat16)], axis=1)
    own = jnp.dot(placing, extended, preferred_element_type=jnp.float32).astype(jnp.bfloat16)
    results = run_experts(own.reshape(2, capacity, width + 128), near, far)
    return lax.dot_general(
        placing, results, (((0,), (0,)), ((), ())), preferred_element_type=jnp.float32
    )


def local(
    queries,
    keys,
    values,
    query_gain,
    key_gain,
    out_weight,
    residual,
    norm_gain,
    route_experts,
    expert_scores,
    group_prob,
    w_gate,
    w_up,
    w_down,
):
    span_tokens = queries.shape[0]
    head_size = key_gain.shape[0]
    local_heads = queries.shape[1] // head_size
    key_heads = keys.shape[1] // head_size
    model_size = lax.axis_size("tp")
    seq_size = lax.axis_size("sp")
    share = local_heads * model_size // key_heads
    model_index = lax.axis_index("tp")
    seq_index = lax.axis_index("sp")
    local_experts = w_gate.shape[0]
    group_experts = local_experts * seq_size // GROUPS
    pairs = (
        local_experts == 1
        and GROUPS == 2
        and group_experts == 2
        and route_experts.shape[1] == 2
        and model_size == 8
    )
    halves = seq_size == 4 and model_size % 2 == 0 and share % (2 * local_heads) == 0

    cosines, sines = rope_tables(seq_index * span_tokens, span_tokens, head_size)
    shared_head = (model_index * local_heads // share).astype(jnp.int32)
    core = (model_index % 2 if halves else 0 * model_index).astype(jnp.int32)
    if pairs:
        near = (w_gate[0], w_up[0], w_down[0])
        far = []
        for block in near:
            far.append(swap(block, 0, 2))
    key_values = prep_keys(
        keys,
        values,
        key_gain,
        cosines,
        sines,
        jnp.stack([shared_head, core]),
        2 if halves else 1,
    )
    if halves:
        fetched = [key_values]
        for bits in (1, 2, 3):
            fetched.append(swap(key_values, bits))
        pieces = fetched + [swap(piece, 0, 1) for piece in fetched]
    else:
        pieces = [lax.all_gather(key_values, "sp", axis=0, tiled=True)]
    attended = attend(queries, query_gain, cosines, sines, pieces)
    all_heads = lax.all_to_all(attended, "tp", split_axis=0, concat_axis=1, tiled=True)
    update = jnp.dot(all_heads, out_weight, preferred_element_type=jnp.float32)
    updated = lax.optimization_barrier((residual.astype(jnp.float32) + update).astype(jnp.bfloat16))
    updated_wide = updated.astype(jnp.float32)
    normed = (
        updated_wide
        * lax.rsqrt(jnp.mean(updated_wide * updated_wide, axis=1, keepdims=True) + norm_eps)
        * norm_gain[None, :]
    ).astype(jnp.bfloat16)
    mixing = group_prob[:, None] * jax.nn.softmax(expert_scores, axis=1)
    if pairs:
        combined = routed_pairs(normed, route_experts, near, far, mixing)
    else:
        combined = routed_general(normed, route_experts, w_gate, w_up, w_down, mixing)
    return (updated_wide + combined).astype(jnp.bfloat16)


def solution(mesh):
    placed = (
        P("sp", "tp"),
        P("sp", None),
        P("sp", None),
        P("tp"),
        P(),
        P(),
        P(("sp", "tp"), None),
        P(),
        P(("sp", "tp"), None),
        P(("sp", "tp"), None),
        P(("sp", "tp")),
        P("sp", None, "tp"),
        P("sp", None, "tp"),
        P("sp", "tp", None),
    )
    return jax.shard_map(
        local, mesh=mesh, in_specs=placed, out_specs=P(("sp", "tp"), None), check_vma=False
    )
```
